32 devices in a mesh: ep: 8 (over z, y), tp: 4 (over x, core).
Axes of the slice: x: 2, y: 2, z: 4, core: 2. Of those that a mesh axis runs over, the one named last changes fastest.
Arguments:
- state_probe_logits: bfloat16 [8192, 1024], P('ep', 'tp'), may hold values from -6 to 6
- retention_logits: bfloat16 [8192, 1024], P('ep', 'tp'), may hold values from -12 to 12
- state_source_entries: bfloat16 [8192, 1024], P('ep', 'tp'), may hold values from -6 to 6
- state_result_switch_logits: bfloat16 [8192, 1024], P('ep', 'tp'), may hold values from -6 to 6
- retention_bound_margin: float32 [1024], P('tp'), may hold values from 0 to 0.07
- extra_fading_amount: float32 [8192, 8], P('ep', 'tp'), may hold values from -0.7 to 0
- state_result_scale: float32 [1024], P('tp'), may hold values from 0.1 to 1.9
- state_result_matrix: bfloat16 [1024, 2048], P(None, 'tp'), may hold values from -0.1875 to 0.1875
- second_slice_tokens: bfloat16 [4096, 2048], P('ep'), may hold values from -6 to 6
- specialist_assignment: int32 [4096, 2], P('ep'), may hold values from 0 to 7, all different within a row; in each aligned block of 128 rows (0 to 127, 128 to 255, ...) at most 64 rows name the same one
- selected_specialist_share: float32 [4096, 2], P('ep'), may hold values from 0.1 to 1
- leading_scale_vector: float32 [2048], replicated, may hold values from 0.1 to 1.9
- trailing_scale_vector: float32 [2048], replicated, may hold values from 0.1 to 1.9
- specialist_switch_matrix: bfloat16 [8, 2048, 2048], P('ep', None, 'tp'), may hold values from -0.3125 to 0.3125
- specialist_widen_matrix: bfloat16 [8, 2048, 2048], P('ep', None, 'tp'), may hold values from -0.3125 to 0.3125
- specialist_contract_matrix: bfloat16 [8, 2048, 2048], P('ep', 'tp'), may hold values from -0.125 to 0.125
Outputs:
- mixer_out: bfloat16 [8192, 2048], P('ep', 'tp')
- moe_out: bfloat16 [4096, 2048], P(('ep', 'tp'))
The draws below stay inside these ranges and needn't reach their ends.
Inputs may be any that keep to these rules, and one draw needn't show every extreme that they name: `specialist_assignment`: each row names 2 different experts. In each aligned block of 128 rows no expert is named by more than 64 rows, a bound that some block reaches.
All inputs are finite; a program needn't handle non-finite values.
Results may differ from the reference program's by a relative error of at most 0.012.
Values may be sent and summed in bfloat16 or wider, within the bound.
A program may use at most 128 MiB of HBM per device.

```python
import math
import jax
import jax.numpy as jnp
import numpy as np
from jax import lax

D = 2048
HEAD = 128
STATE_GROUPS = 8
STATE_FEATURES = 1024
SPAN_STEPS = 64
FFE = 2048
EXPERTS = 8
TOP_K = 2
MIX_EP = 1024
TOK_DEV = 128
MIX_TOKENS = 8192
MOE_TOKENS = 4096
CAPQ = 64
N_TP = 4


def draw_retention_logits(key, part):
    noise_key, shift_key = jax.random.split(key)
    span_rows = max(MIX_EP // 4, 1)
    span_count = MIX_TOKENS // span_rows
    noise = jax.random.normal(noise_key, (MIX_TOKENS, STATE_FEATURES), jnp.float32)
    shifts = jax.random.uniform(shift_key, (span_count,), jnp.float32, -1.0, 1.5)
    return (noise + jnp.repeat(shifts, span_rows)[:, None]).astype(jnp.bfloat16)


def draw_retention_bound_margin(key, part):
    head_key, slow_key, fast_key = jax.random.split(key, 3)
    picked = jax.random.uniform(head_key, (STATE_GROUPS,), jnp.float32)
    slow_heads = picked < 0.5
    slow_channel = jnp.repeat(slow_heads, HEAD)
    lower = math.log(0.5 / MIX_TOKENS)
    upper = math.log(4.0 / MIX_TOKENS)
    slow_gap = jnp.exp(jax.random.uniform(slow_key, (STATE_FEATURES,), jnp.float32, lower, upper))
    fast_gap = jax.random.uniform(fast_key, (STATE_FEATURES,), jnp.float32, 0.03, 0.07)
    return jnp.where(slow_channel, slow_gap, fast_gap)


def draw_extra_fading_amount(key, part):
    where_key, depth_key = jax.random.split(key)
    struck = jax.random.uniform(where_key, (MIX_TOKENS, STATE_GROUPS), jnp.float32) < 6.0 / MIX_TOKENS
    depth = jnp.log(jax.random.uniform(depth_key, (MIX_TOKENS, STATE_GROUPS), jnp.float32, 0.5, 0.8))
    return jnp.where(struck, depth, jnp.zeros((), jnp.float32))


def block_levels(key, dims, pieces, smallest, largest):
    level = 1.0
    for position, shards_of in pieces:
        steps = jax.random.uniform(jax.random.fold_in(jax.random.fold_in(key, 6), position), (shards_of,), jnp.float32, smallest / len(pieces), largest / len(pieces))
        level = level * jnp.repeat(jnp.exp(steps), dims[position] // shards_of).reshape((-1,) + (1,) * (len(dims) - 1 - position))
    return level


def deal_out(key, own, number, rows, count, top, reach, lean):
    order = jax.random.permutation(key, count)
    packed, ordinary = shares(count, rows * top, reach, lean, True), shares(count, rows * top, reach, lean, False)
    places = jnp.arange(count)

    def named(tallies, rotation):
        used = int((tallies > 0).sum())
        fixed = max(1, used // 4)
        passed = fixed + (places - fixed + rotation * (used - fixed)) % max(1, count - fixed)
        return jnp.zeros((count,), jnp.int32).at[order[jnp.where(places < fixed, places, passed)]].set(jnp.asarray(tallies, jnp.int32))

    tallies = jnp.where(number % 4 == 0, named(packed, number // 4), named(ordinary, number - number // 4 - 1))
    mixed = jax.random.permutation(jax.random.fold_in(own, 3), count)
    giver, receiver = mixed[0:count // 2 * 2:2], mixed[1:count // 2 * 2:2]
    slack = jnp.minimum(tallies[giver] - 1, reach - tallies[receiver]) // 2
    slack = jnp.where((giver == order[0]) | (receiver == order[0]) | (tallies[receiver] == 0), 0, jnp.maximum(slack, 0))
    passed = jax.random.randint(jax.random.fold_in(own, 4), (count // 2,), 0, 1 << 20) % (slack + 1)
    tallies = tallies.at[giver].add(-passed).at[receiver].add(passed)
    labels = jnp.searchsorted(jnp.cumsum(tallies), jnp.arange(rows * top), side="right").astype(jnp.int32)
    grid = labels.reshape(top, rows).T
    grid = grid[jax.random.permutation(jax.random.fold_in(own, 1), rows)]
    rotation = jax.random.randint(jax.random.fold_in(own, 2), (rows, 1), 0, top)
    return jnp.take_along_axis(grid, (jnp.arange(top)[None, :] + rotation) % top, axis=1)


def shares(count, total, limit, lean, full):
    weights = [(1 << 20) // math.isqrt(standing ** lean) + 1 for standing in range(1, count + 1)]
    largest = limit if full else min(limit, max(-(-total // count), total * weights[0] // sum(weights)))
    least = 1 if total - largest >= count - 1 else 0
    counts, surplus = [largest] + [least] * (count - 1), total - largest - least * (count - 1)
    while surplus > 0:
        candidates = [i for i in range(1, count) if counts[i] < largest] or [i for i in range(1, count) if counts[i] < limit]
        mass, remaining = sum([weights[i] for i in candidates]), surplus
        for i in candidates:
            addition = min(limit - counts[i], max(1, remaining * weights[i] // mass), surplus)
            counts[i] = counts[i] + addition
            surplus = surplus - addition
    return np.array(counts)


def normal_values(stream_key, shape, scale, most, pieces=(), held_as=jnp.bfloat16):
    drawn = scale * jax.random.normal(stream_key, shape, jnp.float32)
    if pieces:
        drawn = drawn * block_levels(stream_key, shape, pieces, -0.22, 0.18)
    return jnp.clip(drawn, -most, most).astype(held_as)


def setup_inputs(seed: int = 0) -> dict:
    seeds = jax.random.split(jax.random.key(seed), 17)
    state_probe_logits = normal_values(seeds[0], (MIX_TOKENS, STATE_FEATURES), 1.0, 6.0, ((0, 8), (1, 4)))
    retention_logits = draw_retention_logits(jax.random.fold_in(seeds[16], 71), 0)
    state_source_entries = normal_values(seeds[2], (MIX_TOKENS, STATE_FEATURES), 1.0, 6.0, ((0, 8), (1, 4)))
    state_result_switch_logits = normal_values(seeds[3], (MIX_TOKENS, STATE_FEATURES), 1.0, 6.0, ((0, 8), (1, 4)))
    retention_bound_margin = draw_retention_bound_margin(jax.random.fold_in(seeds[16], 71), 0)
    extra_fading_amount = draw_extra_fading_amount(jax.random.fold_in(seeds[16], 71), 0)
    state_result_scale = jnp.clip(1.0 + 0.18 * jax.random.normal(seeds[6], (STATE_FEATURES,), jnp.float32), 0.1, 1.9)
    state_result_matrix = normal_values(seeds[7], (STATE_FEATURES, D), STATE_FEATURES ** -0.5, 0.1875, ((1, 4),))
    second_slice_tokens = normal_values(seeds[8], (MOE_TOKENS, D), 1.0, 6.0, ((0, 8),))
    specialist_assignment_keys = jax.random.split(jax.random.fold_in(seeds[9], 1), MOE_TOKENS // TOK_DEV)
    specialist_assignment_turns = jax.random.permutation(jax.random.fold_in(seeds[9], 3), MOE_TOKENS // TOK_DEV)
    specialist_assignment = jax.vmap(lambda own, number: deal_out(jax.random.fold_in(seeds[9], 2), own, number, TOK_DEV, EXPERTS, TOP_K, CAPQ, 1))(specialist_assignment_keys, specialist_assignment_turns).reshape((MOE_TOKENS, TOP_K))
    selected_specialist_share = jnp.clip(jnp.exp(math.log(1.0) - 2.3025851 * jax.random.uniform(seeds[10], (MOE_TOKENS, TOP_K), jnp.float32) ** block_levels(seeds[10], (MOE_TOKENS, TOP_K), ((0, 8),), -0.2, 0.2)), 0.1, 1.0)
    leading_scale_vector = jnp.clip(1.0 + 0.18 * jax.random.normal(seeds[11], (D,), jnp.float32), 0.1, 1.9)
    trailing_scale_vector = jnp.clip(1.0 + 0.18 * jax.random.normal(seeds[12], (D,), jnp.float32), 0.1, 1.9)
    specialist_switch_matrix = normal_values(seeds[13], (EXPERTS, D, FFE), (D // 6) ** -0.5, 0.3125, ((0, 8), (2, 4)))
    specialist_widen_matrix = normal_values(seeds[14], (EXPERTS, D, FFE), (D // 6) ** -0.5, 0.3125, ((0, 8), (2, 4)))
    specialist_contract_matrix = normal_values(seeds[15], (EXPERTS, FFE, D), FFE ** -0.5, 0.125, ((0, 8), (1, 4)))
    return dict(state_probe_logits=state_probe_logits, retention_logits=retention_logits, state_source_entries=state_source_entries, state_result_switch_logits=state_result_switch_logits, retention_bound_margin=retention_bound_margin, extra_fading_amount=extra_fading_amount, state_result_scale=state_result_scale, state_result_matrix=state_result_matrix, second_slice_tokens=second_slice_tokens, specialist_assignment=specialist_assignment, selected_specialist_share=selected_specialist_share, leading_scale_vector=leading_scale_vector, trailing_scale_vector=trailing_scale_vector, specialist_switch_matrix=specialist_switch_matrix, specialist_widen_matrix=specialist_widen_matrix, specialist_contract_matrix=specialist_contract_matrix)


NORM_EPS = 1e-06
SWISH_ALPHA = 1.702
CLAMP_LIMIT = 7.0
EXACT = lax.Precision.HIGHEST

def rms_scale(values, gain):
    return values * lax.rsqrt(lax.optimization_barrier(jnp.mean(values * values, axis=-1, keepdims=True)) + NORM_EPS) * gain

def clamped_unit(gate, upward):
    glued = jnp.minimum(gate, CLAMP_LIMIT)
    linear = jnp.clip(upward, -CLAMP_LIMIT, CLAMP_LIMIT)
    return glued * jax.nn.sigmoid(SWISH_ALPHA * glued) * (linear + 1.0)

def state_space_layer(state_probe_logits, retention_logits, state_source_entries, state_result_switch_logits, retention_bound_margin, extra_fading_amount, state_result_scale):
    total_rows = state_probe_logits.shape[0]
    span_tally = total_rows // SPAN_STEPS
    causal = jnp.tril(jnp.ones((SPAN_STEPS, SPAN_STEPS), jnp.float32))

    def per_head(values):
        return values.reshape(SPAN_STEPS, STATE_GROUPS, HEAD).transpose(1, 0, 2)

    def advance(state, operand_tensors):
        query_preact, forget_preact, value_preact, micro_batch_rows = operand_tensors
        query = per_head(jax.nn.silu(query_preact.astype(jnp.float32)) * HEAD ** (-0.5))
        input_key = per_head(retention_bound_margin * jax.nn.sigmoid(-forget_preact.astype(jnp.float32)))
        decay_logarithm = jnp.log1p(-input_key) + micro_batch_rows.T[:, :, None]
        values = per_head(value_preact.astype(jnp.float32))
        cumul = jnp.cumsum(decay_logarithm, axis=1)
        middle = cumul[:, SPAN_STEPS // 2 - 1:SPAN_STEPS // 2]
        last = cumul[:, SPAN_STEPS - 1:]
        scores = jnp.einsum('hid,hjd->hij', query * jnp.exp(cumul - middle), input_key * jnp.exp(middle - cumul), precision=EXACT) * causal
        inner = jnp.einsum('hij,hje->hie', scores, values, precision=EXACT)
        outer = jnp.einsum('hid,hde->hie', query * jnp.exp(cumul), state, precision=EXACT)
        update = jnp.einsum('hcd,hce->hde', input_key * jnp.exp(last - cumul), values, precision=EXACT)
        state = jnp.exp(last[:, 0])[:, :, None] * state + update
        return (state, inner + outer)
    operand_tensors = (state_probe_logits.reshape(span_tally, SPAN_STEPS, STATE_FEATURES), retention_logits.reshape(span_tally, SPAN_STEPS, STATE_FEATURES), state_source_entries.reshape(span_tally, SPAN_STEPS, STATE_FEATURES), extra_fading_amount.reshape(span_tally, SPAN_STEPS, STATE_GROUPS))
    final_state, raw_out = lax.scan(advance, jnp.zeros((STATE_GROUPS, HEAD, HEAD), jnp.float32), operand_tensors)
    normed = raw_out * lax.rsqrt(lax.optimization_barrier(jnp.mean(raw_out * raw_out, axis=-1, keepdims=True)) + NORM_EPS)
    normed = normed.transpose(0, 2, 1, 3).reshape(total_rows, STATE_FEATURES)
    return (normed * state_result_scale * jax.nn.silu(state_result_switch_logits.astype(jnp.float32))).astype(jnp.bfloat16)

def experts(second_slice_tokens, specialist_assignment, selected_specialist_share, leading_scale_vector, trailing_scale_vector, specialist_switch_matrix, specialist_widen_matrix, specialist_contract_matrix):
    token_count = second_slice_tokens.shape[0]
    span_tally = token_count // TOK_DEV
    normed = rms_scale(second_slice_tokens.astype(jnp.float32), leading_scale_vector).astype(jnp.bfloat16)
    per_block = TOK_DEV * TOP_K
    flat = specialist_assignment.reshape(span_tally, per_block)
    onehot = (flat[:, :, None] == jnp.arange(EXPERTS, dtype=jnp.int32)[None, None, :]).astype(jnp.int32)
    rank = lax.optimization_barrier(jnp.sum(onehot * (jnp.cumsum(onehot, axis=1) - 1), axis=2))
    slots = ((flat * span_tally + jnp.arange(span_tally, dtype=jnp.int32)[:, None]) * CAPQ + rank).reshape(-1)
    owner = jnp.arange(token_count * TOP_K, dtype=jnp.int32) // TOP_K
    per_expert = span_tally * CAPQ
    room = EXPERTS * per_expert
    source = jnp.zeros((room,), jnp.int32).at[slots].set(owner)
    filled = jnp.zeros((room,), jnp.int32).at[slots].set(1)
    width = FFE // N_TP

    def one_expert(operand_tensors):
        rows_source, rows_live, gate_w, up_w, down_w = operand_tensors
        chosen = jnp.where(rows_live[:, None] > 0, normed[rows_source], jnp.zeros((), jnp.bfloat16))
        gate = jnp.dot(chosen, gate_w, preferred_element_type=jnp.float32)
        upward = jnp.dot(chosen, up_w, preferred_element_type=jnp.float32)
        activated = clamped_unit(gate, upward).astype(jnp.bfloat16)
        parts = jnp.einsum('rjf,jfd->jrd', activated.reshape(per_expert, N_TP, width).astype(jnp.float32), down_w.reshape(N_TP, width, D).astype(jnp.float32))
        parts = lax.optimization_barrier(parts.astype(jnp.bfloat16))
        return lax.optimization_barrier(jnp.sum(parts.astype(jnp.float32), axis=0)).astype(jnp.bfloat16)
    outputs = lax.map(one_expert, (source.reshape(EXPERTS, per_expert), filled.reshape(EXPERTS, per_expert), specialist_switch_matrix, specialist_widen_matrix, specialist_contract_matrix))
    flat_out = outputs.reshape(room, D)
    token_slots = slots.reshape(token_count, TOP_K)
    combined = jnp.zeros((token_count, D), jnp.float32)
    for column in range(TOP_K):
        combined = combined + flat_out[token_slots[:, column]].astype(jnp.float32) * selected_specialist_share[:, column:column + 1]
    return rms_scale(combined, trailing_scale_vector).astype(jnp.bfloat16)

def reference(state_probe_logits, retention_logits, state_source_entries, state_result_switch_logits, retention_bound_margin, extra_fading_amount, state_result_scale, state_result_matrix, second_slice_tokens, specialist_assignment, selected_specialist_share, leading_scale_vector, trailing_scale_vector, specialist_switch_matrix, specialist_widen_matrix, specialist_contract_matrix):
    state_layer_result = state_space_layer(state_probe_logits, retention_logits, state_source_entries, state_result_switch_logits, retention_bound_margin, extra_fading_amount, state_result_scale)
    mixer_out = jnp.dot(state_layer_result, state_result_matrix, preferred_element_type=jnp.float32).astype(jnp.bfloat16)
    moe_out = experts(second_slice_tokens, specialist_assignment, selected_specialist_share, leading_scale_vector, trailing_scale_vector, specialist_switch_matrix, specialist_widen_matrix, specialist_contract_matrix)
    return (mixer_out, moe_out)
```

```python
import functools

import jax
import jax.numpy as jnp
from jax import lax
from jax.experimental import pallas as pl
from jax.experimental.pallas import tpu as pltpu
from jax.sharding import PartitionSpec as P

HEAD = 128
SPAN = 128
TOK_DEV = 128

NORM_EPS = 1e-06
SWISH_ALPHA = 1.702
CLAMP_LIMIT = 7.0
MESH = pl.DeviceIdType.MESH
VMEM = pltpu.VMEM
DMA = pltpu.SemaphoreType.DMA
NT = (((1,), (1,)), ((), ()))
TN = (((0,), (0,)), ((), ()))


def xor(a, b, n):
    total, bit = 0, 1
    while bit < n:
        total = total + ((a // bit + b // bit) % 2) * bit
        bit *= 2
    return total


def places():
    i, j = lax.axis_index("ep"), lax.axis_index("tp")
    mate = j + 1 - 2 * (j % 2)
    cross = (j + 2) % 4
    return i, j, mate, cross


def greet(n, i, j, mate, cross):
    barrier = pltpu.get_barrier_semaphore()

    def one(s, c):
        pl.semaphore_signal(barrier, inc=1, device_id=((i + s) % n, j), device_id_type=MESH)
        return c

    lax.fori_loop(1, n, one, 0)
    for t in (mate, cross):
        pl.semaphore_signal(barrier, inc=1, device_id=(i, t), device_id_type=MESH)
    pl.semaphore_wait(barrier, n + 1)


def remote(src, dst, send, recv, where):
    return pltpu.make_async_remote_copy(
        src_ref=src, dst_ref=dst, send_sem=send, recv_sem=recv, device_id=where, device_id_type=MESH
    )


def span_step(t, probe, ret, val, margin, extra, raw, qdec, state, running):
    rows = pl.ds(pl.multiple_of(t * SPAN, SPAN), SPAN)
    width = probe.shape[1]
    x = probe[rows, :].astype(jnp.float32)
    q = x * jax.nn.sigmoid(x) * HEAD ** (-0.5)
    k = margin[...] * jax.nn.sigmoid(-ret[rows, :].astype(jnp.float32))
    logs = jnp.log1p(-k)
    row = lax.broadcasted_iota(jnp.int32, (SPAN, SPAN), 0)
    col = lax.broadcasted_iota(jnp.int32, (SPAN, SPAN), 1)
    causal = row >= col
    tril = jnp.where(causal, 1.0, 0.0).astype(jnp.float32)
    for h in range(width // HEAD):
        cols = slice(h * HEAD, (h + 1) * HEAD)
        qh, kh = q[:, cols], k[:, cols]
        ld = logs[:, cols] + extra[rows, h : h + 1]
        cum = jnp.dot(
            tril, ld, precision=lax.Precision.HIGHEST, preferred_element_type=jnp.float32
        )
        middle = cum[SPAN // 2 - 1 : SPAN // 2, :]
        last = cum[SPAN - 1 :, :]
        a = (qh * jnp.exp(cum - middle)).astype(jnp.bfloat16)
        b = (kh * jnp.exp(middle - cum)).astype(jnp.bfloat16)
        qe = qh * jnp.exp(cum)
        kd = (kh * jnp.exp(last - cum)).astype(jnp.bfloat16)
        v = val[rows, cols]
        s = lax.dot_general(a, b, NT, preferred_element_type=jnp.float32)
        s = jnp.where(causal, s, 0.0).astype(jnp.bfloat16)
        st = state[h]
        out = jnp.dot(s, v, preferred_element_type=jnp.float32)
        out = out + lax.dot_general(
            qe.astype(jnp.bfloat16), st.astype(jnp.bfloat16), NT, preferred_element_type=jnp.float32
        )
        raw[rows, cols] = out
        before = running[0:1, cols]
        qdec[rows, cols] = (qe * jnp.exp(before)).astype(jnp.bfloat16)
        state[h] = jnp.exp(last) * st + lax.dot_general(
            v, kd, TN, preferred_element_type=jnp.float32
        )
        running[:, cols] = running[:, cols] + last


def dispatch_kernel(
    n, packed, probe, ret, val, margin, extra,
    out, raw, qdec, state_out, running,
    state, asend, arecv, xsend, xrecv, csend, crecv, dsend, drecv, own_sem,
):
    i, j, mate, cross = places()
    spans = probe.shape[0] // SPAN
    greet(n, i, j, mate, cross)

    def direct(s):
        k = xor(i, s, n)
        return remote(packed.at[k], out.at[j, i], asend.at[s], arecv.at[s], (k, j))

    def over_x(src, s):
        k = xor(i, s, n)
        return remote(src, out.at[j, k], xsend.at[s], xrecv.at[s], (i, cross))

    def over_c(src, s):
        k = xor(i, s, n)
        return remote(src, out.at[j, k], csend.at[s], crecv.at[s], (i, mate))

    def over_d(s):
        k = xor(i, s, n)
        return remote(out.at[cross, k], out.at[cross, k], dsend.at[s], drecv.at[s], (i, mate))

    def start_direct(t, c):
        direct(n - 1 - t).start()
        return c

    lax.fori_loop(0, n - 1, start_direct, 0)
    own = pltpu.make_async_copy(packed.at[i], out.at[j, i], own_sem)
    own.start()
    over_x(packed.at[i], 0).start()
    over_c(packed.at[i], 0).start()
    state[...] = jnp.zeros_like(state)
    running[...] = jnp.zeros_like(running)

    def span(t):
        span_step(t, probe, ret, val, margin, extra, raw, qdec, state, running)

    def serve(t, c):
        @pl.when(t < spans)
        def _():
            span(t)

        s = n - 1 - t
        k = xor(i, s, n)
        direct(s).wait_recv()
        over_x(out.at[j, k], s).start()
        over_c(out.at[j, k], s).start()
        before = (s + 1) % n
        over_x(out.at[j, xor(i, before, n)], before).wait_recv()
        over_d(before).start()
        return c

    lax.fori_loop(0, n - 1, serve, 0)

    def rest(t, c):
        span(t)
        return c

    if spans > n - 1:
        lax.fori_loop(n - 1, spans, rest, 0)
    over_x(packed.at[i], 1).wait_recv()
    over_d(1).start()
    own.wait()

    def finish(s, c):
        over_x(packed.at[i], s).wait_send()
        over_c(packed.at[i], s).wait_send()
        over_c(packed.at[i], s).wait_recv()
        over_d(s).wait()
        return c

    lax.fori_loop(0, n, finish, 0)

    def finish_direct(s, c):
        direct(s).wait_send()
        return c

    lax.fori_loop(1, n, finish_direct, 0)
    for h in range(state.shape[0]):
        state_out[h] = state[h].astype(jnp.bfloat16)


def dispatch(n, packed, probe, ret, val, margin, extra):
    rows, width = probe.shape
    heads = width // HEAD
    vm = pl.BlockSpec(memory_space=VMEM)
    hbm = pl.BlockSpec(memory_space=pl.ANY)
    return pl.pallas_call(
        functools.partial(dispatch_kernel, n),
        name="dispatch",
        out_shape=(
            jax.ShapeDtypeStruct((4,) + packed.shape, jnp.bfloat16),
            jax.ShapeDtypeStruct((rows, width), jnp.float32),
            jax.ShapeDtypeStruct((rows, width), jnp.bfloat16),
            jax.ShapeDtypeStruct((heads, HEAD, HEAD), jnp.bfloat16),
            jax.ShapeDtypeStruct((8, width), jnp.float32),
        ),
        in_specs=[vm] * 6,
        out_specs=(hbm, vm, vm, vm, vm),
        scratch_shapes=[VMEM((heads, HEAD, HEAD), jnp.float32)] + [DMA((n,))] * 8 + [DMA],
        compiler_params=pltpu.CompilerParams(
            collective_id=0, has_side_effects=True, vmem_limit_bytes=48 * 2**20
        ),
        cost_estimate=pl.CostEstimate(
            flops=10**9, bytes_accessed=150 * 10**6, transcendentals=10**6
        ),
    )(packed, probe, ret, val, margin, extra)


def mixer_kernel(
    n, chunks, raw, qdec, switch, state, decay, scale, weight,
    out,
    states, decays, gath, enter, ssend, srecv, esend, erecv,
    xsend, xrecv, csend, crecv, dsend, drecv,
):
    i, j, mate, cross = places()
    rows, width = raw.shape
    part = rows // chunks
    heads = width // HEAD
    greet(n, i, j, mate, cross)

    def send_state(s):
        k = (i + s) % n
        return remote(state, states.at[i], ssend.at[s], srecv.at[s], (k, j))

    def send_decay(s):
        k = (i + s) % n
        return remote(decay, decays.at[i], esend.at[s], erecv.at[s], (k, j))

    def begin(s, c):
        send_state(s).start()
        send_decay(s).start()
        return c

    lax.fori_loop(1, n, begin, 0)

    def end(s, c):
        send_state(s).wait()
        send_decay(s).wait()
        return c

    lax.fori_loop(1, n, end, 0)
    enter[...] = jnp.zeros_like(enter)

    def join(p, c):
        @pl.when(p < i)
        def _():
            for h in range(heads):
                d = decays[p, 0:1, h * HEAD : (h + 1) * HEAD]
                enter[h] = jnp.exp(d) * enter[h] + states[p, h].astype(jnp.float32)

        return c

    lax.fori_loop(0, n, join, 0)

    def at(c):
        return pl.ds(pl.multiple_of(c * part, part), part)

    def over_x(c):
        here = gath.at[j, at(c)]
        return remote(here, here, xsend.at[c], xrecv.at[c], (i, cross))

    def over_c(c):
        here = gath.at[j, at(c)]
        return remote(here, here, csend.at[c], crecv.at[c], (i, mate))

    def over_d(c):
        here = gath.at[cross, at(c)]
        return remote(here, here, dsend.at[c], drecv.at[c], (i, mate))

    def final(c, carry):
        r = at(c)
        for h in range(heads):
            cols = slice(h * HEAD, (h + 1) * HEAD)
            x = raw[r, cols] + lax.dot_general(
                qdec[r, cols], enter[h].astype(jnp.bfloat16), NT,
                preferred_element_type=jnp.float32,
            )
            x = x * lax.rsqrt(jnp.mean(x * x, axis=-1, keepdims=True) + NORM_EPS)
            g = switch[r, cols].astype(jnp.float32)
            gath[j, r, cols] = (x * scale[:, cols] * (g * jax.nn.sigmoid(g))).astype(jnp.bfloat16)
        over_x(c).start()
        over_c(c).start()
        return carry

    lax.fori_loop(0, chunks, final, 0)

    def pass_on(c, carry):
        over_x(c).wait()
        over_d(c).start()
        return carry

    lax.fori_loop(0, chunks, pass_on, 0)

    def project(c, carry):
        over_c(c).wait()
        over_d(c).wait()
        r = at(c)
        acc = jnp.dot(gath[0, r, :], weight[0:width, :], preferred_element_type=jnp.float32)
        for p in range(1, 4):
            acc = acc + jnp.dot(
                gath[p, r, :], weight[p * width : (p + 1) * width, :],
                preferred_element_type=jnp.float32,
            )
        out[r, :] = acc.astype(jnp.bfloat16)
        return carry

    lax.fori_loop(0, chunks, project, 0)


def mixer(n, raw, qdec, switch, state, decay, scale, weight):
    rows, width = raw.shape
    heads = width // HEAD
    chunks = 4
    vm = pl.BlockSpec(memory_space=VMEM)
    return pl.pallas_call(
        functools.partial(mixer_kernel, n, chunks),
        name="mixer",
        out_shape=jax.ShapeDtypeStruct((rows, weight.shape[1]), jnp.bfloat16),
        in_specs=[vm] * 7,
        out_specs=vm,
        scratch_shapes=[
            VMEM((n, heads, HEAD, HEAD), jnp.bfloat16),
            VMEM((n, 8, width), jnp.float32),
            VMEM((4, rows, width), jnp.bfloat16),
            VMEM((heads, HEAD, HEAD), jnp.float32),
        ]
        + [DMA((n,))] * 4
        + [DMA((chunks,))] * 6,
        compiler_params=pltpu.CompilerParams(
            collective_id=1, has_side_effects=True, vmem_limit_bytes=48 * 2**20
        ),
        cost_estimate=pl.CostEstimate(
            flops=10**9, bytes_accessed=60 * 10**6, transcendentals=10**6
        ),
    )(raw, qdec, switch, state, decay, scale, weight)


def return_kernel(
    n, part,
    out,
    acc, sendb, recvb, fin, asend0, arecv0, asend1, arecv1, bsend, brecv, rsend, rrecv,
):
    i, j, mate, cross = places()
    mate_cross = (mate + 2) % 4
    greet(n, i, j, mate, cross)

    def to_mate(s, near):
        k = xor(i, s, n)
        if near:
            return remote(part.at[mate, k], acc.at[0, s], asend0.at[s], arecv0.at[s], (i, mate))
        return remote(part.at[mate_cross, k], acc.at[1, s], asend1.at[s], arecv1.at[s], (i, mate))

    def to_cross(s):
        return remote(sendb.at[s], recvb.at[s], bsend.at[s], brecv.at[s], (i, cross))

    def home(s):
        k = xor(i, s, n)
        return remote(fin.at[s], out.at[i], rsend.at[s], rrecv.at[s], (k, j))

    def home_in(s):
        k = xor(i, s, n)
        return remote(fin.at[s], out.at[k], rsend.at[s], rrecv.at[s], (k, j))

    def first(t, c):
        s = n - 1 - t
        to_mate(s, False).start()
        to_mate(s, True).start()
        return c

    lax.fori_loop(0, n, first, 0)

    def second(t, c):
        s = n - 1 - t
        k = xor(i, s, n)
        to_mate(s, False).wait()
        x = part[cross, k].astype(jnp.float32) + acc[1, s].astype(jnp.float32)
        sendb[s] = x.astype(jnp.bfloat16)
        to_cross(s).start()
        return c

    lax.fori_loop(0, n, second, 0)

    def total(s):
        k = xor(i, s, n)
        to_mate(s, True).wait()
        to_cross(s).wait()
        x = part[j, k].astype(jnp.float32) + acc[0, s].astype(jnp.float32)
        return (x + recvb[s].astype(jnp.float32)).astype(jnp.bfloat16)

    def third(t, c):
        s = n - 1 - t
        fin[s] = total(s)
        home(s).start()
        return c

    lax.fori_loop(0, n - 1, third, 0)
    out[i] = total(0)

    def fourth(s, c):
        home(s).wait_send()
        home_in(s).wait_recv()
        return c

    lax.fori_loop(1, n, fourth, 0)


def give_back(n, part):
    shape = part.shape[1:]
    vm = pl.BlockSpec(memory_space=VMEM)
    return pl.pallas_call(
        functools.partial(return_kernel, n),
        name="give_back",
        out_shape=jax.ShapeDtypeStruct(shape, jnp.bfloat16),
        in_specs=[vm],
        out_specs=vm,
        scratch_shapes=[
            VMEM((2,) + shape, jnp.bfloat16),
            VMEM(shape, jnp.bfloat16),
            VMEM(shape, jnp.bfloat16),
            VMEM(shape, jnp.bfloat16),
        ]
        + [DMA((n,))] * 8,
        compiler_params=pltpu.CompilerParams(
            collective_id=2, has_side_effects=True, vmem_limit_bytes=48 * 2**20
        ),
        cost_estimate=pl.CostEstimate(
            flops=10**8, bytes_accessed=150 * 10**6, transcendentals=0
        ),
    )(part)


def rms_scale(values, gain):
    return values * lax.rsqrt(jnp.mean(values * values, axis=-1, keepdims=True) + NORM_EPS) * gain


def clamped_unit(gate, upward):
    glued = jnp.minimum(gate, CLAMP_LIMIT)
    linear = jnp.clip(upward, -CLAMP_LIMIT, CLAMP_LIMIT)
    return glued * jax.nn.sigmoid(SWISH_ALPHA * glued) * (linear + 1.0)


def slot_hits(routes, experts, capacity):
    tokens, top = routes.shape
    ids = jnp.arange(experts, dtype=jnp.int32)
    onehot = (routes[:, :, None] == ids).astype(jnp.float32)
    named = jnp.sum(onehot, axis=1)
    earlier = jnp.tril(jnp.ones((tokens, tokens), jnp.float32), -1)
    ahead = jnp.dot(earlier, named, preferred_element_type=jnp.float32)
    rank = jnp.sum(onehot * ahead[:, None, :], axis=2).astype(jnp.int32)
    slots = routes * capacity + rank
    return slots[:, :, None] == jnp.arange(experts * capacity, dtype=jnp.int32)


def shards(
    state_probe_logits,
    retention_logits,
    state_source_entries,
    state_result_switch_logits,
    retention_bound_margin,
    extra_fading_amount,
    state_result_scale,
    state_result_matrix,
    second_slice_tokens,
    specialist_assignment,
    selected_specialist_share,
    leading_scale_vector,
    trailing_scale_vector,
    specialist_switch_matrix,
    specialist_widen_matrix,
    specialist_contract_matrix,
):
    n = lax.axis_size("ep")
    experts = specialist_switch_matrix.shape[0] * n
    top_count = specialist_assignment.shape[1]
    capacity = 2 * TOK_DEV * top_count // experts
    first = lax.axis_index("tp") * TOK_DEV
    own_route = lax.dynamic_slice_in_dim(specialist_assignment, first, TOK_DEV, 0)
    own_weight = lax.dynamic_slice_in_dim(selected_specialist_share, first, TOK_DEV, 0)
    own_rows = lax.dynamic_slice_in_dim(second_slice_tokens, first, TOK_DEV, 0)
    normed = rms_scale(own_rows.astype(jnp.float32), leading_scale_vector).astype(jnp.bfloat16)
    hits = slot_hits(own_route, experts, capacity)
    pick = jnp.any(hits, axis=1).astype(jnp.bfloat16)
    packed = lax.dot_general(pick, normed, TN, preferred_element_type=jnp.float32)
    packed = packed.astype(jnp.bfloat16).reshape(n, capacity, -1)

    portion, raw, qdec, state, decay = dispatch(
        n,
        packed,
        state_probe_logits,
        retention_logits,
        state_source_entries,
        retention_bound_margin[None, :],
        extra_fading_amount,
    )
    mixer_out = mixer(
        n,
        raw,
        qdec,
        state_result_switch_logits,
        state,
        decay,
        state_result_scale[None, :],
        state_result_matrix,
    )

    rows = portion.reshape(-1, portion.shape[3])
    gate = jnp.dot(rows, specialist_switch_matrix[0], preferred_element_type=jnp.float32)
    upward = jnp.dot(rows, specialist_widen_matrix[0], preferred_element_type=jnp.float32)
    activated = clamped_unit(gate, upward).astype(jnp.bfloat16)
    parts = jnp.dot(
        activated, specialist_contract_matrix[0], preferred_element_type=jnp.float32
    ).astype(jnp.bfloat16)
    returned = give_back(n, parts.reshape(portion.shape))

    flat = returned.reshape(-1, returned.shape[2])
    spread = jnp.sum(jnp.where(hits, own_weight[:, :, None], 0.0), axis=1)
    high = spread.astype(jnp.bfloat16)
    low = (spread - high.astype(jnp.float32)).astype(jnp.bfloat16)
    combined = jnp.dot(high, flat, preferred_element_type=jnp.float32) + jnp.dot(
        low, flat, preferred_element_type=jnp.float32
    )
    moe_out = rms_scale(combined, trailing_scale_vector).astype(jnp.bfloat16)
    return (mixer_out, moe_out)


def solution(mesh):
    return jax.shard_map(
        shards,
        mesh=mesh,
        in_specs=(
            P("ep", "tp"),
            P("ep", "tp"),
            P("ep", "tp"),
            P("ep", "tp"),
            P("tp"),
            P("ep", "tp"),
            P("tp"),
            P(None, "tp"),
            P("ep", None),
            P("ep", None),
            P("ep", None),
            P(),
            P(),
            P("ep", None, "tp"),
            P("ep", None, "tp"),
            P("ep", "tp", None),
        ),
        out_specs=(P("ep", "tp"), P(("ep", "tp"), None)),
        check_vma=False,
    )
```

```python
import functools

import jax
import jax.numpy as jnp
from jax import lax
from jax.experimental import pallas as pl
from jax.experimental.pallas import tpu as pltpu
from jax.sharding import PartitionSpec as P

HEAD = 128
SPAN = 128
TOK_DEV = 128

NORM_EPS = 1e-06
SWISH_ALPHA = 1.702
CLAMP_LIMIT = 7.0
MESH = pl.DeviceIdType.MESH
VMEM = pltpu.VMEM
DMA = pltpu.SemaphoreType.DMA
NT = (((1,), (1,)), ((), ()))
TN = (((0,), (0,)), ((), ()))


def xor(a, b, n):
    total, bit = 0, 1
    while bit < n:
        total = total + ((a // bit + b // bit) % 2) * bit
        bit *= 2
    return total


def places():
    i, j = lax.axis_index("ep"), lax.axis_index("tp")
    mate = j + 1 - 2 * (j % 2)
    cross = (j + 2) % 4
    return i, j, mate, cross


def greet(n, i, j, mate, cross):
    barrier = pltpu.get_barrier_semaphore()

    def one(s, c):
        pl.semaphore_signal(barrier, inc=1, device_id=((i + s) % n, j), device_id_type=MESH)
        return c

    lax.fori_loop(1, n, one, 0)
    for t in (mate, cross):
        pl.semaphore_signal(barrier, inc=1, device_id=(i, t), device_id_type=MESH)
    pl.semaphore_wait(barrier, n + 1)


def remote(src, dst, send, recv, where):
    return pltpu.make_async_remote_copy(
        src_ref=src, dst_ref=dst, send_sem=send, recv_sem=recv, device_id=where, device_id_type=MESH
    )


def span_step(t, probe, ret, val, margin, extra, raw, qdec, state, running):
    rows = pl.ds(pl.multiple_of(t * SPAN, SPAN), SPAN)
    width = probe.shape[1]
    x = probe[rows, :].astype(jnp.float32)
    q = x * jax.nn.sigmoid(x) * HEAD ** (-0.5)
    k = margin[...] * jax.nn.sigmoid(-ret[rows, :].astype(jnp.float32))
    logs = jnp.log1p(-k)
    row = lax.broadcasted_iota(jnp.int32, (SPAN, SPAN), 0)
    col = lax.broadcasted_iota(jnp.int32, (SPAN, SPAN), 1)
    causal = row >= col
    tril = jnp.where(causal, 1.0, 0.0).astype(jnp.float32)
    for h in range(width // HEAD):
        cols = slice(h * HEAD, (h + 1) * HEAD)
        qh, kh = q[:, cols], k[:, cols]
        ld = logs[:, cols] + extra[rows, h : h + 1]
        cum = jnp.dot(
            tril, ld, precision=lax.Precision.HIGHEST, preferred_element_type=jnp.float32
        )
        middle = cum[SPAN // 2 - 1 : SPAN // 2, :]
        last = cum[SPAN - 1 :, :]
        a = (qh * jnp.exp(cum - middle)).astype(jnp.bfloat16)
        b = (kh * jnp.exp(middle - cum)).astype(jnp.bfloat16)
        qe = qh * jnp.exp(cum)
        kd = (kh * jnp.exp(last - cum)).astype(jnp.bfloat16)
        v = val[rows, cols]
        s = lax.dot_general(a, b, NT, preferred_element_type=jnp.float32)
        s = jnp.where(causal, s, 0.0).astype(jnp.bfloat16)
        st = state[h]
        out = jnp.dot(s, v, preferred_element_type=jnp.float32)
        out = out + lax.dot_general(
            qe.astype(jnp.bfloat16), st.astype(jnp.bfloat16), NT, preferred_element_type=jnp.float32
        )
        raw[rows, cols] = out
        before = running[0:1, cols]
        qdec[rows, cols] = (qe * jnp.exp(before)).astype(jnp.bfloat16)
        state[h] = jnp.exp(last) * st + lax.dot_general(
            v, kd, TN, preferred_element_type=jnp.float32
        )
        running[:, cols] = running[:, cols] + last


def moe_kernel(
    n, packed, probe, ret, val, margin, extra, gate_hbm, up_hbm, down_hbm,
    raw, qdec, state_out, running, back,
    state, rows, part, gate_w, up_w, down_w, acc, sendb, recvb, fin,
    asend, arecv, xsend, xrecv, csend, crecv, dsend, drecv, own_sem, weight_sem,
    esend0, erecv0, esend1, erecv1, bsend, brecv, rsend, rrecv,
):
    i, j, mate, cross = places()
    mate_cross = (mate + 2) % 4
    spans = probe.shape[0] // SPAN
    capacity, features = packed.shape[1], packed.shape[2]
    loads = [
        pltpu.make_async_copy(src, dst, weight_sem.at[w])
        for w, (src, dst) in enumerate(((gate_hbm, gate_w), (up_hbm, up_w), (down_hbm, down_w)))
    ]
    for load in loads:
        load.start()
    greet(n, i, j, mate, cross)

    def direct(s):
        k = xor(i, s, n)
        return remote(packed.at[k], rows.at[i, j], asend.at[s], arecv.at[s], (k, j))

    def over_x(src, s):
        k = xor(i, s, n)
        return remote(src, rows.at[k, j], xsend.at[s], xrecv.at[s], (i, cross))

    def over_c(src, s):
        k = xor(i, s, n)
        return remote(src, rows.at[k, j], csend.at[s], crecv.at[s], (i, mate))

    def over_d(s):
        k = xor(i, s, n)
        return remote(rows.at[k, cross], rows.at[k, cross], dsend.at[s], drecv.at[s], (i, mate))

    def to_mate(s, near):
        k = xor(i, s, n)
        if near:
            return remote(part.at[k, mate], acc.at[0, k], esend0.at[s], erecv0.at[s], (i, mate))
        return remote(
            part.at[k, mate_cross], acc.at[1, k], esend1.at[s], erecv1.at[s], (i, mate)
        )

    def to_cross(s):
        return remote(sendb.at[s], recvb.at[s], bsend.at[s], brecv.at[s], (i, cross))

    def home(s):
        k = xor(i, s, n)
        return remote(fin.at[s], back.at[i], rsend.at[s], rrecv.at[s], (k, j))

    def home_in(s):
        k = xor(i, s, n)
        return remote(fin.at[s], back.at[k], rsend.at[s], rrecv.at[s], (k, j))

    def start_direct(t, c):
        direct(n - 1 - t).start()
        return c

    direct(1).start()
    lax.fori_loop(0, n - 2, start_direct, 0)
    own = pltpu.make_async_copy(packed.at[i], rows.at[i, j], own_sem)
    own.start()
    over_x(packed.at[i], 0).start()
    over_c(packed.at[i], 0).start()
    state[...] = jnp.zeros_like(state)
    running[...] = jnp.zeros_like(running)

    def order(t):
        return ((t + n - 1) // n) * (1 + (n - t) % (n - 1))

    def span(t):
        span_step(t, probe, ret, val, margin, extra, raw, qdec, state, running)

    def serve(t):
        s = order(t)
        k = xor(i, s, n)
        direct(s).wait_recv()
        over_x(rows.at[k, j], s).start()
        over_c(rows.at[k, j], s).start()

    def work(t):
        s = order(t)
        k = xor(i, s, n)
        over_c(packed.at[i], s).wait_recv()
        over_d(s).wait_recv()
        x = rows[k].reshape(4 * capacity, features)
        gate = jnp.dot(x, gate_w[...], preferred_element_type=jnp.float32)
        upward = jnp.dot(x, up_w[...], preferred_element_type=jnp.float32)
        act = clamped_unit(gate, upward).astype(jnp.bfloat16)
        step = 512
        for f in range(0, features, step):
            y = jnp.dot(act, down_w[:, f : f + step], preferred_element_type=jnp.float32)
            part[k, :, :, f : f + step] = y.astype(jnp.bfloat16).reshape(4, capacity, step)
        to_mate(s, False).start()
        to_mate(s, True).start()

    def first_sum(t):
        s = order(t)
        k = xor(i, s, n)
        to_mate(s, False).wait()
        x = part[k, cross].astype(jnp.float32) + acc[1, k].astype(jnp.float32)
        sendb[s] = x.astype(jnp.bfloat16)
        to_cross(s).start()

    def total(s):
        k = xor(i, s, n)
        to_mate(s, True).wait()
        to_cross(s).wait()
        x = part[k, j].astype(jnp.float32) + acc[0, k].astype(jnp.float32)
        return (x + recvb[s].astype(jnp.float32)).astype(jnp.bfloat16)

    def pump(t, c):
        @pl.when(t < spans)
        def _():
            span(t)

        @pl.when(t + 1 < n)
        def _():
            serve(t + 1)

        @pl.when(t < n)
        def _():
            s = order(t)
            over_x(packed.at[i], s).wait_recv()
            over_d(s).start()

        @pl.when((t >= 1) & (t < n + 1))
        def _():
            work(t - 1)

        @pl.when((t >= 2) & (t < n + 2))
        def _():
            first_sum(t - 2)

        @pl.when((t >= 4) & (t < n + 3))
        def _():
            s = order(t - 3)
            fin[s] = total(s)
            home(s).start()

        return c

    own.wait()
    for load in loads:
        load.wait()
    lax.fori_loop(0, max(n + 3, spans), pump, 0)
    back[i] = total(0)

    def finish(s, c):
        over_x(packed.at[i], s).wait_send()
        over_c(packed.at[i], s).wait_send()
        over_d(s).wait_send()
        return c

    lax.fori_loop(0, n, finish, 0)

    def finish_direct(s, c):
        direct(s).wait_send()
        home(s).wait_send()
        home_in(s).wait_recv()
        return c

    lax.fori_loop(1, n, finish_direct, 0)
    for h in range(state.shape[0]):
        state_out[h] = state[h].astype(jnp.bfloat16)


def moe(n, packed, probe, ret, val, margin, extra, gate_w, up_w, down_w):
    length, width = probe.shape
    heads = width // HEAD
    vm = pl.BlockSpec(memory_space=VMEM)
    hbm = pl.BlockSpec(memory_space=pl.ANY)
    chunk = packed.shape[1:]
    bf = jnp.bfloat16
    return pl.pallas_call(
        functools.partial(moe_kernel, n),
        name="moe",
        out_shape=(
            jax.ShapeDtypeStruct((length, width), jnp.float32),
            jax.ShapeDtypeStruct((length, width), bf),
            jax.ShapeDtypeStruct((heads, HEAD, HEAD), bf),
            jax.ShapeDtypeStruct((8, width), jnp.float32),
            jax.ShapeDtypeStruct(packed.shape, bf),
        ),
        in_specs=[vm] * 6 + [hbm] * 3,
        out_specs=(vm,) * 5,
        scratch_shapes=[
            VMEM((heads, HEAD, HEAD), jnp.float32),
            VMEM((n, 4) + chunk, bf),
            VMEM((n, 4) + chunk, bf),
            VMEM(gate_w.shape, bf),
            VMEM(up_w.shape, bf),
            VMEM(down_w.shape, bf),
            VMEM((2, n) + chunk, bf),
            VMEM((n,) + chunk, bf),
            VMEM((n,) + chunk, bf),
            VMEM((n,) + chunk, bf),
        ]
        + [DMA((n,))] * 8
        + [DMA, DMA((3,))]
        + [DMA((n,))] * 8,
        compiler_params=pltpu.CompilerParams(
            collective_id=0, has_side_effects=True, vmem_limit_bytes=60 * 2**20
        ),
        cost_estimate=pl.CostEstimate(
            flops=10**10, bytes_accessed=200 * 10**6, transcendentals=10**6
        ),
    )(packed, probe, ret, val, margin, extra, gate_w, up_w, down_w)


def mixer_kernel(
    n, chunks, raw, qdec, switch, state, decay, scale, weight,
    out,
    states, decays, gath, enter, ssend, srecv, esend, erecv,
    xsend, xrecv, csend, crecv, dsend, drecv,
):
    i, j, mate, cross = places()
    rows, width = raw.shape
    part = rows // chunks
    heads = width // HEAD
    greet(n, i, j, mate, cross)

    def send_state(s):
        k = (i + s) % n
        return remote(state, states.at[i], ssend.at[s], srecv.at[s], (k, j))

    def send_decay(s):
        k = (i + s) % n
        return remote(decay, decays.at[i], esend.at[s], erecv.at[s], (k, j))

    def begin(s, c):
        send_state(s).start()
        send_decay(s).start()
        return c

    lax.fori_loop(1, n, begin, 0)

    def end(s, c):
        send_state(s).wait()
        send_decay(s).wait()
        return c

    lax.fori_loop(1, n, end, 0)
    enter[...] = jnp.zeros_like(enter)

    def join(p, c):
        @pl.when(p < i)
        def _():
            for h in range(heads):
                d = decays[p, 0:1, h * HEAD : (h + 1) * HEAD]
                enter[h] = jnp.exp(d) * enter[h] + states[p, h].astype(jnp.float32)

        return c

    lax.fori_loop(0, n, join, 0)

    def at(c):
        return pl.ds(pl.multiple_of(c * part, part), part)

    def over_x(c):
        here = gath.at[j, at(c)]
        return remote(here, here, xsend.at[c], xrecv.at[c], (i, cross))

    def over_c(c):
        here = gath.at[j, at(c)]
        return remote(here, here, csend.at[c], crecv.at[c], (i, mate))

    def over_d(c):
        here = gath.at[cross, at(c)]
        return remote(here, here, dsend.at[c], drecv.at[c], (i, mate))

    def final(c, carry):
        r = at(c)
        for h in range(heads):
            cols = slice(h * HEAD, (h + 1) * HEAD)
            x = raw[r, cols] + lax.dot_general(
                qdec[r, cols], enter[h].astype(jnp.bfloat16), NT,
                preferred_element_type=jnp.float32,
            )
            x = x * lax.rsqrt(jnp.mean(x * x, axis=-1, keepdims=True) + NORM_EPS)
            g = switch[r, cols].astype(jnp.float32)
            gath[j, r, cols] = (x * scale[:, cols] * (g * jax.nn.sigmoid(g))).astype(jnp.bfloat16)
        over_x(c).start()
        over_c(c).start()
        return carry

    lax.fori_loop(0, chunks, final, 0)

    def pass_on(c, carry):
        over_x(c).wait()
        over_d(c).start()
        return carry

    lax.fori_loop(0, chunks, pass_on, 0)

    def project(c, carry):
        over_c(c).wait()
        over_d(c).wait()
        r = at(c)
        acc = jnp.dot(gath[0, r, :], weight[0:width, :], preferred_element_type=jnp.float32)
        for p in range(1, 4):
            acc = acc + jnp.dot(
                gath[p, r, :], weight[p * width : (p + 1) * width, :],
                preferred_element_type=jnp.float32,
            )
        out[r, :] = acc.astype(jnp.bfloat16)
        return carry

    lax.fori_loop(0, chunks, project, 0)


def mixer(n, raw, qdec, switch, state, decay, scale, weight):
    rows, width = raw.shape
    heads = width // HEAD
    chunks = 4
    vm = pl.BlockSpec(memory_space=VMEM)
    return pl.pallas_call(
        functools.partial(mixer_kernel, n, chunks),
        name="mixer",
        out_shape=jax.ShapeDtypeStruct((rows, weight.shape[1]), jnp.bfloat16),
        in_specs=[vm] * 7,
        out_specs=vm,
        scratch_shapes=[
            VMEM((n, heads, HEAD, HEAD), jnp.bfloat16),
            VMEM((n, 8, width), jnp.float32),
            VMEM((4, rows, width), jnp.bfloat16),
            VMEM((heads, HEAD, HEAD), jnp.float32),
        ]
        + [DMA((n,))] * 4
        + [DMA((chunks,))] * 6,
        compiler_params=pltpu.CompilerParams(
            collective_id=1, has_side_effects=True, vmem_limit_bytes=48 * 2**20
        ),
        cost_estimate=pl.CostEstimate(
            flops=10**9, bytes_accessed=60 * 10**6, transcendentals=10**6
        ),
    )(raw, qdec, switch, state, decay, scale, weight)


def rms_scale(values, gain):
    return values * lax.rsqrt(jnp.mean(values * values, axis=-1, keepdims=True) + NORM_EPS) * gain


def clamped_unit(gate, upward):
    glued = jnp.minimum(gate, CLAMP_LIMIT)
    linear = jnp.clip(upward, -CLAMP_LIMIT, CLAMP_LIMIT)
    return glued * jax.nn.sigmoid(SWISH_ALPHA * glued) * (linear + 1.0)


def slot_hits(routes, experts, capacity):
    tokens, top = routes.shape
    ids = jnp.arange(experts, dtype=jnp.int32)
    onehot = (routes[:, :, None] == ids).astype(jnp.float32)
    named = jnp.sum(onehot, axis=1)
    earlier = jnp.tril(jnp.ones((tokens, tokens), jnp.float32), -1)
    ahead = jnp.dot(earlier, named, preferred_element_type=jnp.float32)
    rank = jnp.sum(onehot * ahead[:, None, :], axis=2).astype(jnp.int32)
    slots = routes * capacity + rank
    return slots[:, :, None] == jnp.arange(experts * capacity, dtype=jnp.int32)


def shards(
    state_probe_logits,
    retention_logits,
    state_source_entries,
    state_result_switch_logits,
    retention_bound_margin,
    extra_fading_amount,
    state_result_scale,
    state_result_matrix,
    second_slice_tokens,
    specialist_assignment,
    selected_specialist_share,
    leading_scale_vector,
    trailing_scale_vector,
    specialist_switch_matrix,
    specialist_widen_matrix,
    specialist_contract_matrix,
):
    n = lax.axis_size("ep")
    experts = specialist_switch_matrix.shape[0] * n
    top_count = specialist_assignment.shape[1]
    capacity = 2 * TOK_DEV * top_count // experts
    first = lax.axis_index("tp") * TOK_DEV
    own_route = lax.dynamic_slice_in_dim(specialist_assignment, first, TOK_DEV, 0)
    own_weight = lax.dynamic_slice_in_dim(selected_specialist_share, first, TOK_DEV, 0)
    own_rows = lax.dynamic_slice_in_dim(second_slice_tokens, first, TOK_DEV, 0)
    normed = rms_scale(own_rows.astype(jnp.float32), leading_scale_vector).astype(jnp.bfloat16)
    hits = slot_hits(own_route, experts, capacity)
    pick = jnp.any(hits, axis=1).astype(jnp.bfloat16)
    packed = lax.dot_general(pick, normed, TN, preferred_element_type=jnp.float32)
    packed = packed.astype(jnp.bfloat16).reshape(n, capacity, -1)

    raw, qdec, state, decay, returned = moe(
        n,
        packed,
        state_probe_logits,
        retention_logits,
        state_source_entries,
        retention_bound_margin[None, :],
        extra_fading_amount,
        specialist_switch_matrix[0],
        specialist_widen_matrix[0],
        specialist_contract_matrix[0],
    )
    mixer_out = mixer(
        n,
        raw,
        qdec,
        state_result_switch_logits,
        state,
        decay,
        state_result_scale[None, :],
        state_result_matrix,
    )

    flat = returned.reshape(-1, returned.shape[2])
    spread = jnp.sum(jnp.where(hits, own_weight[:, :, None], 0.0), axis=1)
    high = spread.astype(jnp.bfloat16)
    low = (spread - high.astype(jnp.float32)).astype(jnp.bfloat16)
    combined = jnp.dot(high, flat, preferred_element_type=jnp.float32) + jnp.dot(
        low, flat, preferred_element_type=jnp.float32
    )
    moe_out = rms_scale(combined, trailing_scale_vector).astype(jnp.bfloat16)
    return (mixer_out, moe_out)


def solution(mesh):
    return jax.shard_map(
        shards,
        mesh=mesh,
        in_specs=(
            P("ep", "tp"),
            P("ep", "tp"),
            P("ep", "tp"),
            P("ep", "tp"),
            P("tp"),
            P("ep", "tp"),
            P("tp"),
            P(None, "tp"),
            P("ep", None),
            P("ep", None),
            P("ep", None),
            P(),
            P(),
            P("ep", None, "tp"),
            P("ep", None, "tp"),
            P("ep", "tp", None),
        ),
        out_specs=(P("ep", "tp"), P(("ep", "tp"), None)),
        check_vma=False,
    )
```
